512 devices in a mesh: sp: 64 (over z, y), tp: 8 (over x, core).
Axes of the slice: x: 4, y: 4, z: 16, core: 2. Of those that a mesh axis runs over, the one named last changes fastest.
Arguments:
- resid: bfloat16 [16384, 2048], P(('sp', 'tp')), may hold values from -6 to 6
- queries: bfloat16 [16384, 1024], P('sp', 'tp'), may hold values from -6 to 6
- keys: bfloat16 [512, 16384], P('tp', 'sp'), may hold values from -6 to 6
- values: bfloat16 [512, 16384], P('tp', 'sp'), may hold values from -6 to 6
- log_gates: float32 [16, 16384], P('tp', 'sp'), may hold values from -1640 to 0, as said below
- q_gain: float32 [64], replicated, may hold values from 0.5 to 7
- k_gain: float32 [64], replicated, may hold values from 0.5 to 7
- w_out: bfloat16 [1024, 2048], P('tp'), may hold values from -0.1875 to 0.1875
- mlp_gain: bfloat16 [2048], replicated, may hold values from 0.099609375 to 1.8984375
- w_up: bfloat16 [2048, 8192], P('sp', 'tp'), may hold values from -0.125 to 0.125
- w_down: bfloat16 [8192, 2048], P('tp', 'sp'), may hold values from -0.0625 to 0.0625
Outputs:
- output: bfloat16 [16384, 2048], P(('sp', 'tp'))
The draws below stay inside these ranges and needn't reach their ends.
Inputs may be any that keep to these rules, and one draw needn't show every extreme that they name: `log_gates`: each head's values never rise along positions.
All inputs are finite; a program needn't handle non-finite values.
Results may differ from the reference program's by a relative error of at most 0.018.
The reference program's roundings to bfloat16 on the way count: a program that leaves them out, or rounds other values in their place, can miss the bound.
Values may be sent and summed in bfloat16 or wider, within the bound.
No kernel may reach another device: no remote copies, remote signals or barrier semaphores. Data moves between devices by JAX's collectives and lax.ppermute only.
A program may use at most 64 MiB of HBM per device.

```python
import math
import jax
import jax.numpy as jnp
from jax import lax

D = 2048
QUERY_HEADS = 16
HK = 8
DH = 64
FF = 8192
TOK_DEV = 256
SEQUENCE_TOKENS = 16384
QD = 1024
KD = 512
N_TP = 8


def key_table(key):
    base = jnp.clip(jax.random.normal(jax.random.fold_in(key, 101), (SEQUENCE_TOKENS, KD), jnp.float32), -6.0, 6.0)
    return base


def draw_keys(key, part):
    base = key_table(key)
    return base.T.astype(jnp.bfloat16)


def draw_values(key, part):
    base = jax.random.normal(jax.random.fold_in(key, 121), (KD, SEQUENCE_TOKENS), jnp.float32)
    return jnp.clip(base, -6.0, 6.0).astype(jnp.bfloat16)


def draw_queries(key, part):
    base = jnp.clip(jax.random.normal(jax.random.fold_in(key, 104), (SEQUENCE_TOKENS, QD), jnp.float32), -6.0, 6.0)
    return base.astype(jnp.bfloat16)


def draw_q_gain(key, part):
    return jax.random.uniform(jax.random.fold_in(key, 106), (DH,), jnp.float32, 0.5, 1.5)


def draw_k_gain(key, part):
    return jax.random.uniform(jax.random.fold_in(key, 107), (DH,), jnp.float32, 0.5, 1.5)


def draw_log_gates(key, part):
    share = 0.5
    slow = jax.random.uniform(jax.random.fold_in(key, 111), (QUERY_HEADS,)) < share
    fast_rate = jnp.exp(jax.random.uniform(jax.random.fold_in(key, 112), (QUERY_HEADS, 1), jnp.float32, math.log(1.0 / 50.0), math.log(1.0 / 30.0)))
    blocks = SEQUENCE_TOKENS // TOK_DEV
    block_factor = jnp.exp(jax.random.uniform(jax.random.fold_in(key, 113), (1, blocks, 1), jnp.float32, math.log(0.5), math.log(2.0)))
    rough = jax.random.uniform(jax.random.fold_in(key, 114), (QUERY_HEADS, blocks, TOK_DEV), jnp.float32, 0.5, 1.5)
    raw = (block_factor * rough).reshape(QUERY_HEADS, SEQUENCE_TOKENS)
    slow_total = jax.random.uniform(jax.random.fold_in(key, 115), (QUERY_HEADS, 1), jnp.float32, 0.4, 0.8)
    slow_step = raw * slow_total / jnp.sum(raw, axis=1, keepdims=True)
    fast_step = raw * fast_rate
    advance_loop = jnp.where(slow[:, None], slow_step, fast_step)
    increments = jax.random.randint(jax.random.fold_in(key, 116), (2,), 1, SEQUENCE_TOKENS)
    loss_values = jax.random.uniform(jax.random.fold_in(key, 117), (QUERY_HEADS, 2), jnp.float32, 0.2, 0.5)
    increment_sum = jnp.zeros((QUERY_HEADS, SEQUENCE_TOKENS), jnp.float32).at[:, increments].add(-jnp.log1p(-loss_values))
    return -jnp.cumsum(advance_loop + increment_sum, axis=1)


def steps_of(rng, dims, pieces, smallest, high):
    def one(position, shards_of):
        steps = jax.random.uniform(jax.random.fold_in(jax.random.fold_in(rng, 6), position), (shards_of,), jnp.float32, smallest / len(pieces), high / len(pieces))
        return jnp.repeat(jnp.exp(steps), dims[position] // shards_of).reshape((-1,) + (1,) * (len(dims) - position - 1))

    factor_of = one(*pieces[0])
    for cut in pieces[1:]:
        factor_of = factor_of * one(*cut)
    return factor_of


def bell_draw(rng, dims, scale, most, cuts=(), held_as=jnp.bfloat16):
    values = scale * jax.random.normal(rng, dims, jnp.float32)
    if cuts:
        values = values * steps_of(rng, dims, cuts, -0.22, 0.18)
    return jnp.clip(values, -most, most).astype(held_as)


def setup_inputs(seed: int = 0) -> dict:
    arg_keys = jax.random.split(jax.random.key(seed), 12)
    resid = bell_draw(arg_keys[0], (SEQUENCE_TOKENS, D), 1.0, 6.0, ((0, 512),))
    queries = draw_queries(jax.random.fold_in(arg_keys[11], 71), 0)
    keys = draw_keys(jax.random.fold_in(arg_keys[11], 71), 0)
    values = draw_values(jax.random.fold_in(arg_keys[11], 71), 0)
    log_gates = draw_log_gates(jax.random.fold_in(arg_keys[11], 71), 0)
    q_gain = draw_q_gain(jax.random.fold_in(arg_keys[11], 71), 0)
    k_gain = draw_k_gain(jax.random.fold_in(arg_keys[11], 71), 0)
    w_out = bell_draw(arg_keys[7], (QD, D), QD ** -0.5, 0.1875, ((0, 8),))
    mlp_gain = jnp.clip(1.0 + 0.18 * jax.random.normal(arg_keys[8], (D,), jnp.float32), 0.099609375, 1.8984375).astype(jnp.bfloat16)
    w_up = bell_draw(arg_keys[9], (D, FF), D ** -0.5, 0.125, ((0, 64), (1, 8)))
    w_down = bell_draw(arg_keys[10], (FF, D), FF ** -0.5, 0.0625, ((0, 8), (1, 64)))
    return {"resid": resid, "queries": queries, "keys": keys, "values": values, "log_gates": log_gates, "q_gain": q_gain, "k_gain": k_gain, "w_out": w_out, "mlp_gain": mlp_gain, "w_up": w_up, "w_down": w_down}


EPS = 1e-06

def rms_last(input_values, gain):
    scale = lax.rsqrt(lax.optimization_barrier(jnp.mean(input_values * input_values, axis=-1, keepdims=True)) + EPS)
    return input_values * scale * gain

def reference(resid, queries, keys, values, log_gates, q_gain, k_gain, w_out, mlp_gain, w_up, w_down):
    group = QUERY_HEADS // HK
    query_heads = queries.astype(jnp.float32).reshape(SEQUENCE_TOKENS, QUERY_HEADS, DH)
    qnorm = (rms_last(query_heads, q_gain) * DH ** (-0.5)).astype(jnp.bfloat16).astype(jnp.float32)
    key_heads = keys.astype(jnp.float32).T.reshape(SEQUENCE_TOKENS, HK, DH)
    knorm = rms_last(key_heads, k_gain).astype(jnp.bfloat16).astype(jnp.float32)
    value_heads = values.astype(jnp.float32).T.reshape(SEQUENCE_TOKENS, HK, DH)
    qblock = math.gcd(SEQUENCE_TOKENS, 256)
    key_gates = log_gates.reshape(HK, group, 1, SEQUENCE_TOKENS)
    key_pos = jnp.arange(SEQUENCE_TOKENS, dtype=jnp.int32)

    def one_block(start):
        qrows = lax.dynamic_slice_in_dim(qnorm, start, qblock, 0).reshape(qblock, HK, group, DH)
        qgates = lax.dynamic_slice_in_dim(log_gates, start, qblock, 1).reshape(HK, group, qblock)
        logits = jnp.einsum('qkgd,skd->kgqs', qrows, knorm) + qgates[..., None] - key_gates
        qpos = start + jnp.arange(qblock, dtype=jnp.int32)
        logits = jnp.where(key_pos[None, :] <= qpos[:, None], logits, -jnp.inf)
        top = lax.optimization_barrier(jnp.max(logits, axis=-1, keepdims=True))
        weights = jnp.exp(logits - top)
        denom = lax.optimization_barrier(jnp.sum(weights, axis=-1))
        probs = lax.optimization_barrier(weights.astype(jnp.bfloat16)).astype(jnp.float32)
        summed = jnp.einsum('kgqs,skd->qkgd', probs, value_heads)
        result = summed / jnp.transpose(denom, (2, 0, 1))[..., None]
        return result.reshape(qblock, QD).astype(jnp.bfloat16)
    starts = (jnp.arange(SEQUENCE_TOKENS // qblock) * qblock).astype(jnp.int32)
    attn = lax.map(one_block, starts).reshape(SEQUENCE_TOKENS, QD)
    proj = jnp.dot(attn, w_out, preferred_element_type=jnp.float32)
    mixed = (resid.astype(jnp.float32) + proj).astype(jnp.bfloat16)
    normed = rms_last(mixed.astype(jnp.float32), mlp_gain.astype(jnp.float32)).astype(jnp.bfloat16)
    upward = jnp.dot(normed, w_up, preferred_element_type=jnp.float32)
    act = jnp.square(jax.nn.relu(upward)).astype(jnp.bfloat16)
    width = FF // N_TP
    summed_down = jnp.zeros((SEQUENCE_TOKENS, D), jnp.float32)
    for index in range(N_TP):
        partial_value = jnp.dot(act[:, index * width:(index + 1) * width], w_down[index * width:(index + 1) * width], preferred_element_type=jnp.float32).astype(jnp.bfloat16)
        summed_down = summed_down + lax.optimization_barrier(partial_value).astype(jnp.float32)
    return (mixed.astype(jnp.float32) + summed_down).astype(jnp.bfloat16)
```

```python
import functools

import jax
import jax.numpy as jnp
from jax import lax
from jax.experimental import pallas as pl
from jax.experimental.pallas import tpu as pltpu
from jax.sharding import Mesh, PartitionSpec as P


EPS = 1e-06
NZ, NY, NX, NC = 16, 4, 4, 2
NTP = NX * NC
NK, NQ = 8, 8
PAIR = 2
MATES = PAIR * NTP
HEAD = 64
HEADS = 2
WIDE = HEADS * HEAD
TOK = 256
ROWS = 32
GATE = 16
KV_ROWS = 2 * HEAD + GATE
CHUNK = 4
PADS = CHUNK - 1
LOW = -1e30
F32 = jnp.float32
BF16 = jnp.bfloat16
VMEM = pl.BlockSpec(memory_space=pltpu.VMEM)
SMEM = pl.BlockSpec(memory_space=pltpu.SMEM)


def three_parts(value):
    high = value.astype(BF16).astype(F32)
    middle = (value - high).astype(BF16).astype(F32)
    low = (value - high - middle).astype(BF16).astype(F32)
    return [high, middle, low]


def parts_of_heads(rows):
    filler = jnp.zeros((GATE // HEADS - 3, TOK), F32)
    return jnp.concatenate([p for row in rows for p in (*three_parts(row), filler)], axis=0)


def prep_kernel(q_ref, k_ref, v_ref, gates_ref, qg_ref, kg_ref, up_ref, down_ref, q_out, kv_out, pair_out):
    half = up_ref.shape[1] // PAIR
    for n in range(NY):
        columns = slice((n % PAIR) * half, (n % PAIR + 1) * half)
        pair_out[n, 0] = up_ref[:, columns]
        pair_out[n, 1] = down_ref[:, columns]
    q = q_ref[...].astype(F32)
    halves = []
    for h in range(HEADS):
        part = q[:, h * HEAD : (h + 1) * HEAD]
        scale = lax.rsqrt(jnp.mean(part * part, axis=-1, keepdims=True) + EPS)
        halves.append(part * scale * qg_ref[...] * HEAD ** (-0.5))
    qn = jnp.concatenate(halves, axis=1).T.astype(BF16)
    for member in range(NQ):
        q_out[member] = qn
    row = lax.broadcasted_iota(jnp.int32, (HEAD, HEAD), 0)
    col = lax.broadcasted_iota(jnp.int32, (HEAD, HEAD), 1)
    k_gain = jnp.sum(jnp.where(row == col, kg_ref[...], 0.0), axis=1, keepdims=True)
    k = k_ref[...].astype(F32)
    scale = lax.rsqrt(jnp.mean(k * k, axis=0, keepdims=True) + EPS)
    kv_out[:HEAD] = (k * scale * k_gain).astype(BF16)
    kv_out[HEAD : HEAD + GATE] = parts_of_heads([-gates_ref[h : h + 1] for h in range(HEADS)]).astype(BF16)
    kv_out[HEAD + GATE :] = v_ref[...]


def attention_kernel(place_ref, q_ref, kv_ref, out_ref, keys_ref, vals_ref, qh_ref, m_ref, l_ref, acc_ref):
    slab = place_ref[0]
    member = place_ref[1]
    lane = lax.broadcasted_iota(jnp.int32, (TOK, WIDE), 1)
    nothing = jnp.where((lane == HEAD) | (lane == HEAD + GATE // HEADS), LOW, 0.0).astype(BF16)
    for j in range(PADS):
        keys_ref[j * TOK : (j + 1) * TOK] = nothing
    vals_ref[:, : PADS * TOK] = jnp.zeros((HEAD, PADS * TOK), BF16)
    rest = jnp.zeros((WIDE - HEAD - GATE, TOK), F32)
    for j in range(NK):
        rows = jnp.concatenate([kv_ref[j, : HEAD + GATE].astype(F32), rest], axis=0)
        where = slice((PADS + j) * TOK, (PADS + j + 1) * TOK)
        keys_ref[where] = rows.T.astype(BF16)
        vals_ref[:, where] = kv_ref[j, HEAD + GATE :]
    spot = lax.broadcasted_iota(jnp.int32, (WIDE - HEAD, TOK), 0)
    for h in range(HEADS):
        first = h * (GATE // HEADS)
        ones = jnp.where((spot >= first) & (spot < first + 3), 1.0, 0.0)
        qh_ref[HEAD:, h * TOK : (h + 1) * TOK] = ones.astype(BF16)

    def one_step(block, back, last):
        start = pl.multiple_of((slab - back * CHUNK) * TOK, TOK)
        s = jnp.dot(keys_ref[pl.ds(start, CHUNK * TOK)], qh_ref[...], preferred_element_type=F32)
        if last:
            key = lax.broadcasted_iota(jnp.int32, (TOK, HEADS * TOK), 0)
            query = lax.broadcasted_iota(jnp.int32, (TOK, HEADS * TOK), 1) & (TOK - 1)
            tail = jnp.where(key - query <= (block - member) * TOK, s[PADS * TOK :], LOW)
            s = jnp.concatenate([s[: PADS * TOK], tail], axis=0)
        new = jnp.max(s, axis=0, keepdims=True)
        if not last:
            old = m_ref[...]
            new = jnp.maximum(old, new)
            factor = jnp.exp(old - new)
        m_ref[...] = new
        p = jnp.exp(s - jnp.maximum(new, LOW * 0.5))
        total = jnp.sum(p, axis=0, keepdims=True)
        product = jnp.dot(vals_ref[:, pl.ds(start, CHUNK * TOK)], p.astype(BF16), preferred_element_type=F32)
        l_ref[...] = total if last else l_ref[...] * factor + total
        acc_ref[...] = product if last else acc_ref[...] * factor + product

    def one_block(block, carry):
        for h in range(HEADS):
            qh_ref[:HEAD, h * TOK : (h + 1) * TOK] = q_ref[block, h * HEAD : (h + 1) * HEAD]
        one_step(block, 0, True)

        def step(c, inner):
            one_step(block, c, False)
            return inner

        lax.fori_loop(1, slab // CHUNK + 1, step, 0)
        l = l_ref[...]
        some = l > 0.0
        safe = jnp.where(some, l, 1.0)
        out = (acc_ref[...] / safe).astype(BF16)
        lse = jnp.where(some, m_ref[...] + jnp.log(safe), LOW)
        for h in range(HEADS):
            out_ref[block, h * HEAD : (h + 1) * HEAD] = out[:, h * TOK : (h + 1) * TOK]
        rows = [lse[:, h * TOK : (h + 1) * TOK] for h in range(HEADS)]
        out_ref[block, WIDE:] = parts_of_heads(rows).astype(BF16)
        return carry

    lax.fori_loop(0, NQ, one_block, 0)


def merge_kernel(in_ref, out_ref):
    tails = [in_ref[n, WIDE:].astype(F32) for n in range(NQ)]
    halves = []
    for h in range(HEADS):
        a = h * (GATE // HEADS)
        sums = [t[a : a + 1] + t[a + 1 : a + 2] + t[a + 2 : a + 3] for t in tails]
        top = functools.reduce(jnp.maximum, sums)
        shares = [jnp.exp(v - top) for v in sums]
        denom = functools.reduce(jnp.add, shares)
        total = None
        for n in range(NQ):
            part = in_ref[n, h * HEAD : (h + 1) * HEAD].astype(F32) * shares[n]
            total = part if total is None else total + part
        halves.append(total / denom)
    attn = jnp.concatenate(halves, axis=0).T.astype(BF16)
    for n in range(MATES):
        out_ref[n] = attn


def ffn_kernel(
    place_ref, attn_ref, near_ref, far_ref, gain_ref, weight_ref,
    mixed_out, keep_out, send_out, total_ref, resid_ref, act_ref, up_ref, down_ref, sem,
):
    step = pl.program_id(0)
    x, core, mate = place_ref[0], place_ref[1], place_ref[2]
    span = weight_ref.shape[2]

    def copies(side):
        where = (up_ref, down_ref)[side]
        return [
            pltpu.make_async_copy(weight_ref.at[z, side], where.at[pl.ds(z * span, span)], sem.at[side, z])
            for z in range(NZ)
        ]

    @pl.when(step == 0)
    def _():
        for side in range(2):
            for copy in copies(side):
                copy.start()

    shift = jnp.where(step == 1, NX - 1, jnp.where(step == 2, 1, jnp.where(step == 3, 2, 0)))
    there = lax.rem(x + shift, NX)
    here = there * NC + core
    other = there * NC + (1 - core)
    right = jnp.concatenate([near_ref[0, :WIDE], far_ref[0, :WIDE]], axis=0)
    for t in range(PAIR):
        left = jnp.concatenate([attn_ref[t * NTP + here], attn_ref[t * NTP + other]], axis=1)
        part = jnp.dot(left, right, preferred_element_type=F32)
        rows = slice(t * TOK, (t + 1) * TOK)

        @pl.when(step == 0)
        def _():
            total_ref[rows] = part

        @pl.when(step > 0)
        def _():
            total_ref[rows] += part

    for source, index in ((near_ref, here), (far_ref, other)):
        for k in range(PAIR):
            token = jnp.where(k == 0, mate, 1 - mate)
            at = pl.multiple_of(token * TOK + index * ROWS, ROWS)
            resid_ref[pl.ds(at, ROWS)] = source[0, WIDE + k * ROWS : WIDE + (k + 1) * ROWS]

    @pl.when(step == NX - 1)
    def _():
        mixed = (resid_ref[...].astype(F32) + total_ref[...]).astype(BF16)
        resid_ref[...] = mixed
        own = pl.multiple_of(mate * TOK + (x * NC + core) * ROWS, ROWS)
        mixed_out[...] = resid_ref[pl.ds(own, ROWS)]
        wide = mixed.astype(F32)
        scale = lax.rsqrt(jnp.mean(wide * wide, axis=-1, keepdims=True) + EPS)
        normed = (wide * scale * gain_ref[...].astype(F32)).astype(BF16)
        for copy in copies(0):
            copy.wait()
        up = jnp.dot(normed, up_ref[...], preferred_element_type=F32)
        act_ref[...] = jnp.square(jnp.maximum(up, 0.0)).astype(BF16)
        for copy in copies(1):
            copy.wait()
        for out, side in ((send_out, 1 - core), (keep_out, core)):
            pieces = []
            for t in range(PAIR):
                for n in range(NX):
                    at = pl.multiple_of(t * TOK + n * NC * ROWS + side * ROWS, ROWS)
                    pieces.append(act_ref[pl.ds(at, ROWS)])
            out[...] = lax.dot_general(
                jnp.concatenate(pieces, axis=0), down_ref[...], (((1,), (1,)), ((), ())), preferred_element_type=F32
            ).astype(BF16)


def call(kernel, shapes, smem=0, count=0, scratch=()):
    return pl.pallas_call(
        kernel,
        out_shape=shapes,
        in_specs=[SMEM] * smem + [VMEM] * count,
        out_specs=jax.tree.map(lambda _: VMEM, shapes),
        scratch_shapes=list(scratch),
    )


def attention(place, q_all, kv):
    return call(
        attention_kernel,
        jax.ShapeDtypeStruct((NQ, KV_ROWS, TOK), BF16),
        smem=1,
        count=2,
        scratch=(
            pltpu.VMEM(((NK + PADS) * TOK, WIDE), BF16),
            pltpu.VMEM((HEAD, (NK + PADS) * TOK), BF16),
            pltpu.VMEM((WIDE, HEADS * TOK), BF16),
            pltpu.VMEM((1, HEADS * TOK), F32),
            pltpu.VMEM((1, HEADS * TOK), F32),
            pltpu.VMEM((HEAD, HEADS * TOK), F32),
        ),
    )(place, q_all, kv)


def ffn(place, attn_all, near, far, gain, weights):
    model = near.shape[2]
    width = weights.shape[3]
    around = pl.BlockSpec((1, near.shape[1], model), lambda r: (r, 0, 0))
    return pl.pallas_call(
        ffn_kernel,
        grid=(NX,),
        out_shape=(jax.ShapeDtypeStruct((ROWS, model), BF16), *[jax.ShapeDtypeStruct((TOK, model), BF16)] * 2),
        in_specs=[SMEM, VMEM, around, around, VMEM, pl.BlockSpec(memory_space=pl.ANY)],
        out_specs=(VMEM, VMEM, VMEM),
        scratch_shapes=[
            pltpu.VMEM((PAIR * TOK, model), F32),
            pltpu.VMEM((PAIR * TOK, model), BF16),
            pltpu.VMEM((PAIR * TOK, width), BF16),
            pltpu.VMEM((model, width), BF16),
            pltpu.VMEM((model, width), BF16),
            pltpu.SemaphoreType.DMA((2, NZ)),
        ],
        name="ffn",
    )(place, attn_all, near, far, gain, weights)


def ring(count, step):
    return [(i, (i + step) % count) for i in range(count)]


def inside(resid, queries, keys, values, log_gates, q_gain, k_gain, w_out, mlp_gain, w_up, w_down):
    model = resid.shape[1]
    half = w_up.shape[1] // PAIR
    columns = ("yh", "yl")
    members = ("zq", *columns)
    mates = ("yl", "x", "c")

    theirs = lax.ppermute(resid, "yl", ring(PAIR, 1))
    q_sent, kv_sent, pair = call(
        prep_kernel,
        (
            jax.ShapeDtypeStruct((NQ, WIDE, TOK), BF16),
            jax.ShapeDtypeStruct((KV_ROWS, TOK), BF16),
            jax.ShapeDtypeStruct((NY, 2, ROWS, half), BF16),
        ),
        count=8,
    )(queries, keys, values, log_gates, q_gain.reshape(1, HEAD), k_gain.reshape(1, HEAD), w_up, w_down.T)
    pair = lax.all_to_all(pair, columns, 0, 0, tiled=True)
    pair = jnp.moveaxis(pair, 0, 1).reshape(1, 2, NY * ROWS, half)
    weights = lax.all_gather(pair, ("zp", "zq"), axis=0, tiled=True)

    own = jnp.concatenate([w_out, resid, theirs], axis=0)
    arrived = [own]
    for step in (1, -1, 2):
        arrived.append(lax.ppermute(own, "x", ring(NX, step)))
    near = jnp.stack(arrived, axis=0)
    far = lax.ppermute(near, "c", ring(NC, 1))

    q_all = lax.all_to_all(q_sent, members, 0, 0, tiled=True)
    kv = lax.all_gather(kv_sent[None], "zp", axis=0, tiled=True)

    place = jnp.stack([lax.axis_index("zp"), lax.axis_index(members)]).astype(jnp.int32)
    partial = attention(place, q_all, kv)
    partial = lax.all_to_all(partial, members, 0, 0, tiled=True)
    attn = call(merge_kernel, jax.ShapeDtypeStruct((MATES, TOK, WIDE), BF16), count=1)(partial)
    attn_all = lax.all_to_all(attn, mates, 0, 0, tiled=True)
    spot = jnp.stack([lax.axis_index("x"), lax.axis_index("c"), lax.axis_index("yl")]).astype(jnp.int32)
    mixed, keep, send = ffn(spot, attn_all, near, far, mlp_gain.reshape(1, model), weights)
    got = lax.ppermute(send, "c", ring(NC, 1))
    both = (keep.astype(F32) + got.astype(F32)).astype(BF16)
    parts = lax.all_to_all(both.reshape(PAIR * NX, ROWS, model), ("yl", "x"), 0, 0, tiled=True)
    return (mixed.astype(F32) + jnp.sum(parts.astype(F32), axis=0)).astype(BF16)


def solution(mesh):
    fine = Mesh(
        mesh.devices.reshape(NK, NZ // NK, NY // PAIR, PAIR, NX, NC), ("zp", "zq", "yh", "yl", "x", "c")
    )
    sp, tp = ("zp", "zq", "yh", "yl"), ("x", "c")
    return jax.shard_map(
        inside,
        mesh=fine,
        in_specs=(
            P((*sp, *tp), None),
            P(sp, tp),
            P(tp, sp),
            P(tp, sp),
            P(tp, sp),
            P(),
            P(),
            P(tp, None),
            P(),
            P(sp, tp),
            P(tp, sp),
        ),
        out_specs=P((*sp, *tp), None),
        check_vma=False,
    )
```
